32 devices in a mesh: grp: 1, ep: 32 (over z, y, x, core).
Axes of the slice: x: 2, y: 2, z: 4, core: 2. Of those that a mesh axis runs over, the one named last changes fastest.
Arguments:
- tokens: bfloat16 [768, 2048], P(('grp', 'ep')), may hold values from -24 to 24, as said below
- routes: int32 [768, 2], P(('grp', 'ep')), may hold values from 0 to 3, all different within a row; in each aligned block of 24 rows (0 to 23, 24 to 47, ...) at most 24 rows name the same one
- gates: float32 [768, 2], P(('grp', 'ep')), may hold values from 0.2 to 1
- w_gate: bfloat16 [32, 2048, 704], P('ep'), may hold values from -0.125 to 0.125
- w_up: bfloat16 [32, 2048, 704], P('ep'), may hold values from -0.125 to 0.125
- w_down: bfloat16 [32, 704, 2048], P('ep'), may hold values from -0.078125 to 0.078125
- norm_gain: float32 [2048], P('ep'), may hold values from 0.1 to 1.9
- norm_bias: float32 [2048], P('ep'), may hold values from -3 to 3
Outputs:
- normed: bfloat16 [768, 2048], P('grp', 'ep')
The draws below stay inside these ranges and needn't reach their ends.
Inputs may be any that keep to these rules, and one draw needn't show every extreme that they name: `routes`: in each aligned block of 24 rows (the rows of one index of ep) no expert is named by more than 24 rows, a bound that some block reaches. `tokens`: feature scales vary across the width.
All inputs are finite; a program needn't handle non-finite values.
Results may differ from the reference program's by a relative error of at most 0.0032.
Values may be sent and summed in bfloat16 or wider, within the bound.
No kernel may reach another device: no remote copies, remote signals or barrier semaphores. Data moves between devices by JAX's collectives and lax.ppermute only.
A program may use at most 192 MiB of HBM per device.

```python
import math
import jax
import jax.numpy as jnp
import numpy as np
from jax import lax

D = 2048
FF = 5632
SPAN = 8
TOP_K = 2
TOK_DEV = 24
HID_DEV = 704
EXPERTS = 4
TOKENS = 768
CAP = 24
N_EP = 32


def draw_tokens(key, part):
    first = jax.random.fold_in(key, 0)
    columns = jnp.arange(D, dtype=jnp.float32)
    scale = 1.0 + 2.0 * columns / (D - 1.0)
    values = jax.random.normal(first, (TOKENS, D), jnp.float32)
    values = jnp.clip(values, -6.0, 6.0)
    return (values * scale[None, :]).astype(jnp.bfloat16)


def block_scale(stream_key, extent, cuts, least, largest):
    def one(position, shards_of):
        draws = jax.random.uniform(jax.random.fold_in(jax.random.fold_in(stream_key, 6), position), (shards_of,), jnp.float32, least / len(cuts), largest / len(cuts))
        return jnp.repeat(jnp.exp(draws), extent[position] // shards_of).reshape((-1,) + (1,) * (len(extent) - position - 1))

    loudness = one(*cuts[0])
    for cut in cuts[1:]:
        loudness = loudness * one(*cut)
    return loudness


def shared_out(own_key, own, number, rows, count, top, reach, slope):
    sequence = jax.random.permutation(own_key, count)
    heavy_load, ordinary = load_shares(count, rows * top, reach, slope, True), load_shares(count, rows * top, reach, slope, False)
    places = jnp.arange(count)

    def named(sizes, offset_by):
        used = int((sizes > 0).sum())
        fixed = max(1, used // 4)
        moved = fixed + (places - fixed + offset_by * (used - fixed)) % max(1, count - fixed)
        return jnp.zeros((count,), jnp.int32).at[sequence[jnp.where(places < fixed, places, moved)]].set(jnp.asarray(sizes, jnp.int32))

    sizes = jnp.where(number % 4 == 0, named(heavy_load, number // 4), named(ordinary, number - number // 4 - 1))
    mixed = jax.random.permutation(jax.random.fold_in(own, 3), count)
    donor, receiver = mixed[0:count // 2 * 2:2], mixed[1:count // 2 * 2:2]
    margin = jnp.minimum(sizes[donor] - 1, reach - sizes[receiver]) // 2
    margin = jnp.where((donor == sequence[0]) | (receiver == sequence[0]) | (sizes[receiver] == 0), 0, jnp.maximum(margin, 0))
    moved = jax.random.randint(jax.random.fold_in(own, 4), (count // 2,), 0, 1 << 20) % (margin + 1)
    sizes = sizes.at[donor].add(-moved).at[receiver].add(moved)
    members = jnp.searchsorted(jnp.cumsum(sizes), jnp.arange(rows * top), side="right").astype(jnp.int32)
    grid = members.reshape(top, rows).T
    grid = grid[jax.random.permutation(jax.random.fold_in(own, 1), rows)]
    offset_by = jax.random.randint(jax.random.fold_in(own, 2), (rows, 1), 0, top)
    return jnp.take_along_axis(grid, (jnp.arange(top)[None, :] + offset_by) % top, axis=1)


def load_shares(amount, total, reach, slope, full):
    portions = [(1 << 20) // math.isqrt(standing ** slope) + 1 for standing in range(1, amount + 1)]
    largest = reach if full else min(reach, max(-(-total // amount), total * portions[0] // sum(portions)))
    least = 1 if total - largest >= amount - 1 else 0
    holding, rest = [largest] + [least] * (amount - 1), total - largest - least * (amount - 1)
    while rest > 0:
        free = [i for i in range(1, amount) if holding[i] < largest] or [i for i in range(1, amount) if holding[i] < reach]
        pool, remaining = sum([portions[i] for i in free]), rest
        for i in free:
            extra = min(reach - holding[i], max(1, remaining * portions[i] // pool), rest)
            holding[i] = holding[i] + extra
            rest = rest - extra
    return np.array(holding)


def normal_values(stream_key, shape, scale, reach, cuts=(), kind=jnp.bfloat16):
    entries = scale * jax.random.normal(stream_key, shape, jnp.float32)
    if cuts:
        entries = entries * block_scale(stream_key, shape, cuts, -0.22, 0.18)
    return jnp.clip(entries, -reach, reach).astype(kind)


def setup_inputs(seed: int = 0, part: int = 0) -> dict:
    seeds = jax.random.split(jax.random.key(seed), 9)
    part_splits = jax.random.split(jax.random.fold_in(seeds[8], part), 9)
    tokens = draw_tokens(jax.random.fold_in(jax.random.fold_in(seeds[8], part), 71), part)
    routes_keys = jax.random.split(jax.random.fold_in(part_splits[1], 1), TOKENS // TOK_DEV)
    routes_turns = jax.random.permutation(jax.random.fold_in(part_splits[1], 3), TOKENS // TOK_DEV)
    routes = jax.vmap(lambda own, number: shared_out(jax.random.fold_in(part_splits[1], 2), own, number, TOK_DEV, EXPERTS, TOP_K, CAP, 2))(routes_keys, routes_turns).reshape((TOKENS, TOP_K))
    gates = jnp.clip(0.2 + 0.8 * jax.random.uniform(part_splits[2], (TOKENS, TOP_K), jnp.float32) ** block_scale(part_splits[2], (TOKENS, TOP_K), ((0, 32),), -0.2, 0.2), 0.2, 1.0)
    w_gate = normal_values(seeds[3], (EXPERTS * SPAN, D, HID_DEV), D ** -0.5, 0.125, ((0, 32),))
    w_up = normal_values(seeds[4], (EXPERTS * SPAN, D, HID_DEV), D ** -0.5, 0.125, ((0, 32),))
    w_down = normal_values(seeds[5], (EXPERTS * SPAN, HID_DEV, D), FF ** -0.5, 0.078125, ((0, 32),))
    norm_gain = jnp.clip(1.0 + 0.18 * jax.random.normal(seeds[6], (D,), jnp.float32), 0.1, 1.9)
    norm_bias = normal_values(seeds[7], (D,), 0.5, 3.0, ((0, 32),), jnp.float32)
    return {"tokens": tokens, "routes": routes, "gates": gates, "w_gate": w_gate, "w_up": w_up, "w_down": w_down, "norm_gain": norm_gain, "norm_bias": norm_bias}


ALPHA = 8.0 ** 0.25
LN_EPS = 1e-05

def reference(tokens, routes, gates, w_gate, w_up, w_down, norm_gain, norm_bias):
    pairs = TOKENS * TOP_K
    flat_routes = routes.reshape(pairs)
    flat_gates = gates.reshape(pairs)
    positions = jnp.arange(pairs, dtype=jnp.int32)
    most_rows = N_EP * CAP

    def one_expert(expert, total):
        start = (expert * SPAN).astype(jnp.int32)
        wg = jnp.transpose(lax.dynamic_slice_in_dim(w_gate, start, SPAN, 0), (1, 0, 2)).reshape(D, FF)
        wu = jnp.transpose(lax.dynamic_slice_in_dim(w_up, start, SPAN, 0), (1, 0, 2)).reshape(D, FF)
        wd = lax.dynamic_slice_in_dim(w_down, start, SPAN, 0).reshape(FF, D)
        keys = jnp.where(flat_routes == expert, 0, pairs).astype(jnp.int32) + positions
        order = jnp.argsort(keys)[:most_rows].astype(jnp.int32)
        valid = flat_routes[order] == expert
        weight = jnp.where(valid, flat_gates[order], jnp.float32(0.0))
        token_rows = (order // TOP_K).astype(jnp.int32)
        picked = tokens[token_rows]
        gate_pre = jnp.dot(picked, wg, preferred_element_type=jnp.float32)
        up_pre = jnp.dot(picked, wu, preferred_element_type=jnp.float32)
        hidden = (jax.nn.silu(gate_pre) * up_pre).astype(jnp.bfloat16)
        result = jnp.dot(hidden, wd, preferred_element_type=jnp.float32)
        return total.at[token_rows].add(result * weight[:, None])
    mixed = lax.fori_loop(0, EXPERTS, one_expert, jnp.zeros((TOKENS, D), jnp.float32))
    summed = ALPHA * tokens.astype(jnp.float32) + mixed
    mean = lax.optimization_barrier(jnp.mean(summed, axis=1, keepdims=True))
    var = lax.optimization_barrier(jnp.mean(summed * summed, axis=1, keepdims=True)) - mean * mean
    normed = (summed - mean) * lax.rsqrt(var + LN_EPS) * norm_gain[None, :] + norm_bias[None, :]
    return normed.astype(jnp.bfloat16)
```

```python
import jax
import jax.numpy as jnp
from jax import lax
from jax.sharding import PartitionSpec as P

SPAN = 8


ALPHA = 8.0**0.25
LN_EPS = 1e-05


def ffn(rows_in, w_gate, w_up, w_down):
    gate_pre = jnp.dot(rows_in, w_gate, preferred_element_type=jnp.float32)
    up_pre = jnp.dot(rows_in, w_up, preferred_element_type=jnp.float32)
    hidden = (jax.nn.silu(gate_pre) * up_pre).astype(jnp.bfloat16)
    return jnp.dot(hidden, w_down, preferred_element_type=jnp.float32)


def on_device(tokens, routes, gates, w_gate, w_up, w_down, norm_gain, norm_bias):
    rows, width = tokens.shape
    devices = lax.axis_size("ep")
    me = lax.axis_index("ep")
    experts = devices // SPAN
    my_expert = me // SPAN
    columns = width // devices
    peers = range(2, SPAN, 2)

    def along(k):
        return [(i, (i + k * SPAN) % devices) for i in range(devices)]

    def across(m):
        return [(i, i ^ m) for i in range(devices)]

    line = [tokens] + [lax.ppermute(tokens, "ep", along(k)) for k in range(1, experts)]
    line = jnp.concatenate(line, axis=0)
    own = [line] + [lax.ppermute(line, "ep", across(m)) for m in peers]
    own = jnp.concatenate(own, axis=0)
    other = lax.ppermute(own, "ep", across(1))

    kept = ffn(own, w_gate[0], w_up[0], w_down[0])
    given = ffn(other, w_gate[0], w_up[0], w_down[0]).astype(jnp.bfloat16)
    summed = kept + lax.ppermute(given, "ep", across(1)).astype(jnp.float32)
    summed = summed.reshape(SPAN // 2, experts * rows, width)
    result = summed[0]
    for slot, m in enumerate(peers):
        part = summed[slot + 1].astype(jnp.bfloat16)
        result = result + lax.ppermute(part, "ep", across(m)).astype(jnp.float32)
    result = result.reshape(experts, rows, width)

    def weight(k):
        named = routes == (my_expert + k) % experts
        return jnp.sum(jnp.where(named, gates, jnp.float32(0.0)), axis=1, keepdims=True)

    z = ALPHA * tokens.astype(jnp.float32) + weight(0) * result[0]
    for k in range(1, experts):
        back = lax.ppermute(result[k].astype(jnp.bfloat16), "ep", along(-k))
        z = z + weight(k) * back.astype(jnp.float32)
    mean = jnp.mean(z, axis=1, keepdims=True)
    var = jnp.mean(z * z, axis=1, keepdims=True) - mean * mean
    normed = (z - mean) * lax.rsqrt(var + LN_EPS)
    normed = normed.reshape(rows, devices, columns).transpose(1, 0, 2)
    normed = lax.all_to_all(normed, "ep", 0, 0, tiled=True).reshape(devices * rows, columns)
    return (normed * norm_gain[None, :] + norm_bias[None, :]).astype(jnp.bfloat16)


def solution(mesh):
    placed = (
        P(("grp", "ep"), None),
        P(("grp", "ep"), None),
        P(("grp", "ep"), None),
        P("ep", None, None),
        P("ep", None, None),
        P("ep", None, None),
        P("ep"),
        P("ep"),
    )
    return jax.shard_map(
        on_device, mesh=mesh, in_specs=placed, out_specs=P("grp", "ep"), check_vma=False
    )
```

```python
import functools

import jax
import jax.numpy as jnp
from jax import lax
from jax.experimental import pallas as pl
from jax.experimental.pallas import tpu as pltpu
from jax.sharding import PartitionSpec as P


SPAN = 8


ALPHA = 8.0**0.25
LN_EPS = 1e-05
STEPS = 4
NT = (((1,), (1,)), ((), ()))


def ffn_kernel(n_own, n_other, *refs):
    n = n_own + n_other
    blocks, (wg, wu, wd, kept, given, gate, up, hidden) = refs[:n], refs[n:]
    step = pl.program_id(0)
    depth = wg.shape[1]

    def rows_at(k):
        return jnp.concatenate([b[:, pl.ds(k * depth, depth)] for b in blocks], axis=0)

    for k in range(STEPS):

        @pl.when(step == k)
        def _(k=k):
            x = rows_at(k)
            g = lax.dot_general(x, wg[...], NT, preferred_element_type=jnp.float32)
            u = lax.dot_general(x, wu[...], NT, preferred_element_type=jnp.float32)
            if k:
                g = g + gate[...]
                u = u + up[...]
            if k < STEPS - 1:
                gate[...] = g
                up[...] = u
            else:
                hidden[...] = (g / (1.0 + jnp.exp(-g)) * u).astype(jnp.bfloat16)

    @pl.when(step >= STEPS)
    def _():
        y = jnp.dot(hidden[...], wd[...], preferred_element_type=jnp.float32)
        split = kept.shape[0]
        kept[...] = y[:split]
        given[...] = y[split:].astype(jnp.bfloat16)


def ffn(own, other, w_gate, w_up, w_down):
    rows, width = own[0].shape
    hid = w_gate.shape[1]
    n_own, n_other = rows * len(own), rows * len(other)
    total = n_own + n_other
    depth = width // STEPS
    first = lambda s: jnp.minimum(s, STEPS - 1)
    second = lambda s: jnp.maximum(s - STEPS, 0)
    whole = pl.BlockSpec((rows, width), lambda s: (0, 0))
    return pl.pallas_call(
        functools.partial(ffn_kernel, len(own), len(other)),
        grid=(2 * STEPS,),
        in_specs=[whole] * (len(own) + len(other))
        + [
            pl.BlockSpec((None, hid, depth), lambda s: (0, 0, first(s))),
            pl.BlockSpec((None, hid, depth), lambda s: (0, 0, first(s))),
            pl.BlockSpec((None, hid, depth), lambda s: (0, 0, second(s))),
        ],
        out_specs=[
            pl.BlockSpec((n_own, depth), lambda s: (0, second(s))),
            pl.BlockSpec((n_other, depth), lambda s: (0, second(s))),
        ],
        out_shape=[
            jax.ShapeDtypeStruct((n_own, width), jnp.float32),
            jax.ShapeDtypeStruct((n_other, width), jnp.bfloat16),
        ],
        scratch_shapes=[
            pltpu.VMEM((total, hid), jnp.float32),
            pltpu.VMEM((total, hid), jnp.float32),
            pltpu.VMEM((total, hid), jnp.bfloat16),
        ],
        cost_estimate=pl.CostEstimate(
            flops=6 * total * width * hid,
            bytes_accessed=6 * width * hid + 8 * total * width,
            transcendentals=total * hid,
        ),
        compiler_params=pltpu.CompilerParams(vmem_limit_bytes=40 << 20),
        name="ffn",
    )(*own, *other, w_gate, w_up, w_down)


def on_device(tokens, routes, gates, w_gate, w_up, w_down, norm_gain, norm_bias):
    rows, width = tokens.shape
    devices = lax.axis_size("ep")
    me = lax.axis_index("ep")
    experts = devices // SPAN
    my_expert = me // SPAN
    columns = width // devices
    peers = list(range(2, SPAN, 2))

    def along(k):
        return [(i, (i + k * SPAN) % devices) for i in range(devices)]

    def across(x, m):
        return lax.ppermute(x, "ep", [(i, i ^ m) for i in range(devices)])

    weights = (w_gate.transpose(0, 2, 1), w_up.transpose(0, 2, 1), w_down)

    line = [tokens] + [lax.ppermute(tokens, "ep", along(k)) for k in range(1, experts)]
    line = jnp.concatenate(line, axis=0)
    remote = {m: across(line, m) for m in peers}
    line_other = across(line, 1)
    kept_own, given = ffn([line], [line_other], *weights)
    kept_own = kept_own + across(given, 1).astype(jnp.float32)

    near, far = peers[:2], peers[2:]
    parts = {}
    for group in (near, far):
        own = [remote[m] for m in group]
        other = [across(r, 1) for r in own]
        kept, given = ffn(own, other, *weights)
        summed = (kept + across(given, 1).astype(jnp.float32)).astype(jnp.bfloat16)
        for i, m in enumerate(group):
            part = summed[i * experts * rows : (i + 1) * experts * rows]
            parts[m] = across(part, m)

    result = kept_own
    for m in peers:
        result = result + parts[m].astype(jnp.float32)
    result = result.reshape(experts, rows, width)

    def weight(k):
        named = routes == (my_expert + k) % experts
        return jnp.sum(jnp.where(named, gates, jnp.float32(0.0)), axis=1, keepdims=True)

    z = ALPHA * tokens.astype(jnp.float32) + weight(0) * result[0]
    for k in range(1, experts):
        back = lax.ppermute(result[k].astype(jnp.bfloat16), "ep", along(-k))
        z = z + weight(k) * back.astype(jnp.float32)
    mean = jnp.mean(z, axis=1, keepdims=True)
    var = jnp.mean(z * z, axis=1, keepdims=True) - mean * mean
    normed = (z - mean) * lax.rsqrt(var + LN_EPS)
    normed = normed.reshape(rows, devices, columns).transpose(1, 0, 2)
    normed = lax.all_to_all(normed, "ep", 0, 0, tiled=True).reshape(devices * rows, columns)
    return (normed * norm_gain[None, :] + norm_bias[None, :]).astype(jnp.bfloat16)


def solution(mesh):
    placed = (
        P(("grp", "ep"), None),
        P(("grp", "ep"), None),
        P(("grp", "ep"), None),
        P("ep", None, None),
        P("ep", None, None),
        P("ep", None, None),
        P("ep"),
        P("ep"),
    )
    return jax.shard_map(
        on_device, mesh=mesh, in_specs=placed, out_specs=P("grp", "ep"), check_vma=False
    )
```

```python
import functools

import jax
import jax.numpy as jnp
from jax import lax
from jax.experimental import pallas as pl
from jax.experimental.pallas import tpu as pltpu
from jax.sharding import PartitionSpec as P


SPAN = 8


ALPHA = 8.0**0.25
LN_EPS = 1e-05
CUT = 256
LANES = 128
NT = (((1,), (1,)), ((), ()))


def load_kernel(n, *refs):
    sources, targets, sems = refs[:n], refs[n : 2 * n], refs[2 * n]
    copies = [
        pltpu.make_async_copy(a.at[0], b, sems.at[i])
        for i, (a, b) in enumerate(zip(sources, targets, strict=True))
    ]
    for copy in copies:
        copy.start()
    for copy in copies:
        copy.wait()


def load(*weights):
    n = len(weights)
    weights = [pltpu.with_memory_space_constraint(w, pltpu.HBM) for w in weights]
    return pl.pallas_call(
        functools.partial(load_kernel, n),
        in_specs=[pl.BlockSpec(memory_space=pltpu.HBM)] * n,
        out_specs=[pl.BlockSpec(memory_space=pltpu.VMEM)] * n,
        out_shape=[jax.ShapeDtypeStruct(w.shape[1:], w.dtype) for w in weights],
        scratch_shapes=[pltpu.SemaphoreType.DMA((n,))],
        compiler_params=pltpu.CompilerParams(vmem_limit_bytes=24 << 20),
        name="load",
    )(*weights)


def ffn_kernel(n, *refs):
    blocks, (wg, wu, wd, kept, given, hidden) = refs[:n], refs[n:]
    hid, width = wg.shape
    x = jnp.concatenate([b[...] for b in blocks], axis=0)
    for j in range(0, hid, CUT):
        cols = slice(j, min(j + CUT, hid))
        g = lax.dot_general(x, wg[cols, :], NT, preferred_element_type=jnp.float32)
        u = lax.dot_general(x, wu[cols, :], NT, preferred_element_type=jnp.float32)
        hidden[:, cols] = (g / (1.0 + jnp.exp(-g)) * u).astype(jnp.bfloat16)
    split = kept.shape[0]
    h = hidden[...]
    for j in range(0, width, CUT):
        cols = slice(j, min(j + CUT, width))
        y = jnp.dot(h, wd[:, cols], preferred_element_type=jnp.float32)
        kept[:, cols] = y[:split]
        given[:, cols] = y[split:].astype(jnp.bfloat16)


def ffn(own, other, w_gate, w_up, w_down):
    hid, width = w_gate.shape
    n_own, n_other = (sum(b.shape[0] for b in group) for group in (own, other))
    total = n_own + n_other
    blocks = [*own, *other]
    on_chip = pl.BlockSpec(memory_space=pltpu.VMEM)
    return pl.pallas_call(
        functools.partial(ffn_kernel, len(blocks)),
        in_specs=[on_chip] * (len(blocks) + 3),
        out_specs=[on_chip] * 2,
        out_shape=[
            jax.ShapeDtypeStruct((n_own, width), jnp.float32),
            jax.ShapeDtypeStruct((n_other, width), jnp.bfloat16),
        ],
        scratch_shapes=[pltpu.VMEM((total, hid), jnp.bfloat16)],
        cost_estimate=pl.CostEstimate(
            flops=6 * total * width * hid,
            bytes_accessed=6 * width * hid + 8 * total * width,
            transcendentals=total * hid,
        ),
        compiler_params=pltpu.CompilerParams(vmem_limit_bytes=24 << 20),
        name="ffn",
    )(*blocks, w_gate, w_up, w_down)


def shares_kernel(experts, expert, routes, gates, out):
    first = expert[0]
    spot = lax.broadcasted_iota(jnp.int32, out.shape, 1)
    wanted = lax.rem(first + spot, experts)
    total = jnp.zeros(out.shape, jnp.float32)
    for k in range(routes.shape[1]):
        named = (routes[:, k : k + 1] == wanted) & (spot < experts)
        total = total + jnp.where(named, gates[:, k : k + 1], jnp.float32(0.0))
    out[...] = total


def shares(expert, routes, gates, experts):
    on_chip = pl.BlockSpec(memory_space=pltpu.VMEM)
    return pl.pallas_call(
        functools.partial(shares_kernel, experts),
        in_specs=[pl.BlockSpec(memory_space=pltpu.SMEM), on_chip, on_chip],
        out_specs=on_chip,
        out_shape=jax.ShapeDtypeStruct((routes.shape[0], LANES), jnp.float32),
        compiler_params=pltpu.CompilerParams(vmem_limit_bytes=4 << 20),
        name="shares",
    )(expert, routes, gates)


def on_device(tokens, routes, gates, w_gate, w_up, w_down, norm_gain, norm_bias):
    rows, width = tokens.shape
    devices = lax.axis_size("ep")
    me = lax.axis_index("ep")
    experts = devices // SPAN
    columns = width // devices
    peers = list(range(2, SPAN, 2))
    others = range(1, experts)

    def along(x, k):
        return lax.ppermute(
            x, "ep", [(i, (i + k * SPAN) % devices) for i in range(devices)]
        )

    def across(x, m):
        return lax.ppermute(x, "ep", [(i, i ^ m) for i in range(devices)])

    weights = load(w_gate.transpose(0, 2, 1), w_up.transpose(0, 2, 1), w_down)

    def run(own):
        other = [across(x, 1) for x in own]
        kept, given = ffn(own, other, *weights)
        return kept + across(given, 1).astype(jnp.float32)

    line = jnp.concatenate([along(tokens, k) for k in others], axis=0)
    home = [tokens] + [across(tokens, m) for m in peers]
    remote = {m: across(line, m) for m in peers}
    result = run([line])

    span = line.shape[0]
    parts = {}
    for group in (peers[:2], peers[2:]):
        summed = run([remote[m] for m in group]).astype(jnp.bfloat16)
        for i, m in enumerate(group):
            parts[m] = across(summed[i * span : (i + 1) * span], m)
    for m in peers:
        result = result + parts[m].astype(jnp.float32)
    back = [
        along(result[(k - 1) * rows : k * rows].astype(jnp.bfloat16), -k)
        for k in others
    ]

    summed = run([jnp.concatenate(home, axis=0)])
    mine = summed[:rows]
    for i, m in enumerate(peers):
        part = summed[(i + 1) * rows : (i + 2) * rows].astype(jnp.bfloat16)
        mine = mine + across(part, m).astype(jnp.float32)

    weight = shares(me.reshape(1) // SPAN, routes, gates, experts)

    z = ALPHA * tokens.astype(jnp.float32) + weight[:, :1] * mine
    for k in others:
        z = z + weight[:, k : k + 1] * back[k - 1].astype(jnp.float32)
    mean = jnp.mean(z, axis=1, keepdims=True)
    var = jnp.mean(z * z, axis=1, keepdims=True) - mean * mean
    normed = (z - mean) * lax.rsqrt(var + LN_EPS)
    normed = normed.reshape(rows, devices, columns).transpose(1, 0, 2)
    normed = lax.all_to_all(normed, "ep", 0, 0, tiled=True).reshape(devices * rows, columns)
    return (normed * norm_gain[None, :] + norm_bias[None, :]).astype(jnp.bfloat16)


def solution(mesh):
    placed = (
        P(("grp", "ep"), None),
        P(("grp", "ep"), None),
        P(("grp", "ep"), None),
        P("ep", None, None),
        P("ep", None, None),
        P("ep", None, None),
        P("ep"),
        P("ep"),
    )
    return jax.shard_map(
        on_device, mesh=mesh, in_specs=placed, out_specs=P("grp", "ep"), check_vma=False
    )
```

```python
import functools

import jax
import jax.numpy as jnp
from jax import lax
from jax.experimental import pallas as pl
from jax.experimental.pallas import tpu as pltpu
from jax.sharding import PartitionSpec as P


SPAN = 8


ALPHA = 8.0**0.25
LN_EPS = 1e-05
CUT = 256
NT = (((1,), (1,)), ((), ()))


def load_kernel(n, *refs):
    sources, targets, sems = refs[:n], refs[n : 2 * n], refs[2 * n]
    copies = [
        pltpu.make_async_copy(a.at[0], b, sems.at[i])
        for i, (a, b) in enumerate(zip(sources, targets, strict=True))
    ]
    for copy in copies:
        copy.start()
    for copy in copies:
        copy.wait()


def load(*weights):
    n = len(weights)
    weights = [pltpu.with_memory_space_constraint(w, pltpu.HBM) for w in weights]
    return pl.pallas_call(
        functools.partial(load_kernel, n),
        in_specs=[pl.BlockSpec(memory_space=pltpu.HBM)] * n,
        out_specs=[pl.BlockSpec(memory_space=pltpu.VMEM)] * n,
        out_shape=[jax.ShapeDtypeStruct(w.shape[1:], w.dtype) for w in weights],
        scratch_shapes=[pltpu.SemaphoreType.DMA((n,))],
        compiler_params=pltpu.CompilerParams(vmem_limit_bytes=2 << 20),
        name="load",
    )(*weights)


def ffn_kernel(n, *refs):
    blocks, (wg, wu, wd, kept, given, hidden) = refs[:n], refs[n:]
    hid, width = wg.shape
    x = jnp.concatenate([b[...] for b in blocks], axis=0)
    for j in range(0, hid, CUT):
        cols = slice(j, min(j + CUT, hid))
        g = lax.dot_general(x, wg[cols, :], NT, preferred_element_type=jnp.float32)
        u = lax.dot_general(x, wu[cols, :], NT, preferred_element_type=jnp.float32)
        hidden[:, cols] = (g / (1.0 + jnp.exp(-g)) * u).astype(jnp.bfloat16)
    split = kept.shape[0]
    h = hidden[...]
    for j in range(0, width, CUT):
        cols = slice(j, min(j + CUT, width))
        y = jnp.dot(h, wd[:, cols], preferred_element_type=jnp.float32)
        kept[:, cols] = y[:split]
        given[:, cols] = y[split:].astype(jnp.bfloat16)


def ffn(own, other, w_gate, w_up, w_down):
    hid, width = w_gate.shape
    n_own, n_other = (sum(b.shape[0] for b in group) for group in (own, other))
    total = n_own + n_other
    blocks = [*own, *other]
    on_chip = pl.BlockSpec(memory_space=pltpu.VMEM)
    return pl.pallas_call(
        functools.partial(ffn_kernel, len(blocks)),
        in_specs=[on_chip] * (len(blocks) + 3),
        out_specs=[on_chip] * 2,
        out_shape=[
            jax.ShapeDtypeStruct((n_own, width), jnp.float32),
            jax.ShapeDtypeStruct((n_other, width), jnp.bfloat16),
        ],
        scratch_shapes=[pltpu.VMEM((total, hid), jnp.bfloat16)],
        cost_estimate=pl.CostEstimate(
            flops=6 * total * width * hid,
            bytes_accessed=6 * width * hid + 8 * total * width,
            transcendentals=total * hid,
        ),
        compiler_params=pltpu.CompilerParams(vmem_limit_bytes=10 << 20),
        name="ffn",
    )(*blocks, w_gate, w_up, w_down)


def shares_kernel(experts, routes, gates, out):
    first = lax.div(lax.axis_index("ep"), SPAN)
    for k in range(experts):
        named = routes[...] == lax.rem(first + k, experts)
        share = jnp.where(named, gates[...], jnp.float32(0.0))
        out[k : k + 1, :] = jnp.sum(share, axis=0, keepdims=True)


def shares(routes, gates, experts):
    on_chip = pl.BlockSpec(memory_space=pltpu.VMEM)
    return pl.pallas_call(
        functools.partial(shares_kernel, experts),
        in_specs=[on_chip, on_chip],
        out_specs=on_chip,
        out_shape=jax.ShapeDtypeStruct((experts, routes.shape[1]), jnp.float32),
        compiler_params=pltpu.CompilerParams(vmem_limit_bytes=2 << 20),
        name="shares",
    )(routes, gates)


def close_kernel(ks, rows, base, one, two, arrived, *outs):
    for i, (k, out) in enumerate(zip(ks, outs, strict=True)):
        total = base[k * rows : (k + 1) * rows, :]
        for part, at in ((one, k - 1), (two, k - 1), (arrived, i)):
            total = total + part[at * rows : (at + 1) * rows, :].astype(jnp.float32)
        out[...] = total.astype(jnp.bfloat16)


def close(ks, rows, base, parts, arrived):
    on_chip = pl.BlockSpec(memory_space=pltpu.VMEM)
    out = jax.ShapeDtypeStruct((rows, base.shape[1]), jnp.bfloat16)
    return pl.pallas_call(
        functools.partial(close_kernel, tuple(ks), rows),
        in_specs=[on_chip] * 4,
        out_specs=[on_chip] * len(ks),
        out_shape=[out] * len(ks),
        compiler_params=pltpu.CompilerParams(vmem_limit_bytes=4 << 20),
        name="close",
    )(base, *parts, arrived)


def on_device(tokens, routes, gates, w_gate, w_up, w_down, norm_gain, norm_bias):
    rows, width = tokens.shape
    devices = lax.axis_size("ep")
    experts = devices // SPAN
    columns = width // devices
    peers = list(range(2, SPAN, 2))
    others = range(1, experts)

    def along(x, k):
        return lax.ppermute(
            x, "ep", [(i, (i + k * SPAN) % devices) for i in range(devices)]
        )

    def across(x, m):
        return lax.ppermute(x, "ep", [(i, i ^ m) for i in range(devices)])

    projections = load(w_gate.transpose(0, 2, 1), w_up.transpose(0, 2, 1))
    weights = (*projections, *load(w_down))

    def run(own):
        other = [across(x, 1) for x in own]
        kept, given = ffn(own, other, *weights)
        return kept + across(given, 1).astype(jnp.float32)

    blocks = [tokens] + [along(tokens, k) for k in others]
    half = experts // 2
    first, second, far = peers
    early = jnp.concatenate(blocks[:half], axis=0)
    late = jnp.concatenate(blocks[half:], axis=0)
    remote = {m: (across(early, m), across(late, m)) for m in (first, second)}
    result = run([early, late])

    upper = across(remote[first][0], second)
    lower = across(remote[second][1], first)

    ahead = range(half, half + experts // 4)
    behind = [k for k in others if k not in ahead]

    def pick(x, ks):
        return jnp.concatenate([x[k * rows : (k + 1) * rows] for k in ks], axis=0)

    summed = {
        m: run(halves).astype(jnp.bfloat16)
        for m, halves in (
            (first, remote[first]), (second, remote[second]), (far, (upper, lower))
        )
    }
    put = {m: across(summed[m][rows:], m) for m in (first, second)}
    put_lead = across(pick(summed[far], ahead), far)
    put_tail = across(pick(summed[far], behind), far)

    back = {}
    for ks, arrived in ((ahead, put_lead), (behind, put_tail)):
        sums = close(ks, rows, result, [put[first], put[second]], arrived)
        for k, total in zip(ks, sums, strict=True):
            back[k] = along(total, -k)
    mine = result[:rows]
    for m in peers:
        mine = mine + across(summed[m][:rows], m).astype(jnp.float32)

    weight = shares(routes.T, gates.T, experts)

    z = ALPHA * tokens.astype(jnp.float32) + weight[0][:, None] * mine
    for k in others:
        z = z + weight[k][:, None] * back[k].astype(jnp.float32)
    mean = jnp.mean(z, axis=1, keepdims=True)
    var = jnp.mean(z * z, axis=1, keepdims=True) - mean * mean
    normed = (z - mean) * lax.rsqrt(var + LN_EPS)
    normed = normed.reshape(rows, devices, columns).transpose(1, 0, 2)
    normed = lax.all_to_all(normed, "ep", 0, 0, tiled=True).reshape(devices * rows, columns)
    return (normed * norm_gain[None, :] + norm_bias[None, :]).astype(jnp.bfloat16)


def solution(mesh):
    placed = (
        P(("grp", "ep"), None),
        P(("grp", "ep"), None),
        P(("grp", "ep"), None),
        P("ep", None, None),
        P("ep", None, None),
        P("ep", None, None),
        P("ep"),
        P("ep"),
    )
    return jax.shard_map(
        on_device, mesh=mesh, in_specs=placed, out_specs=P("grp", "ep"), check_vma=False
    )
```

```python
import functools

import jax
import jax.numpy as jnp
from jax import lax
from jax.experimental import pallas as pl
from jax.experimental.pallas import tpu as pltpu
from jax.sharding import PartitionSpec as P


SPAN = 8


ALPHA = 8.0**0.25
LN_EPS = 1e-05
TN = (((0,), (0,)), ((), ()))
CUT = 256
CHUNKS = 4
LANES = 128
NT = (((1,), (1,)), ((), ()))


def load_kernel(n, *refs):
    sources, targets, sems = refs[:n], refs[n : 2 * n], refs[2 * n]
    copies = []
    for i, (source, target) in enumerate(zip(sources, targets, strict=True)):
        step = target.shape[0] // CHUNKS if target.shape[0] % (16 * CHUNKS) == 0 else target.shape[0]
        for c in range(target.shape[0] // step):
            part = pl.ds(c * step, step)
            copies.append(pltpu.make_async_copy(source.at[part], target.at[part], sems.at[i, c]))
    for copy in copies:
        copy.start()
    for copy in copies:
        copy.wait()


def load(*arrays):
    n = len(arrays)
    arrays = [pltpu.with_memory_space_constraint(x, pltpu.HBM) for x in arrays]
    return pl.pallas_call(
        functools.partial(load_kernel, n),
        in_specs=[pl.BlockSpec(memory_space=pltpu.HBM)] * n,
        out_specs=[pl.BlockSpec(memory_space=pltpu.VMEM)] * n,
        out_shape=[jax.ShapeDtypeStruct(x.shape, x.dtype) for x in arrays],
        scratch_shapes=[pltpu.SemaphoreType.DMA((n, CHUNKS))],
        compiler_params=pltpu.CompilerParams(vmem_limit_bytes=2 << 20),
        name="load",
    )(*arrays)


def ffn_kernel(n, *refs):
    blocks, (wg, wu, wd, kept, given, hidden) = refs[:n], refs[n:]
    hid, width = wg.shape
    x = jnp.concatenate([b[...] for b in blocks], axis=0)
    for j in range(0, hid, CUT):
        cols = slice(j, min(j + CUT, hid))
        g = lax.dot_general(x, wg[cols, :], NT, preferred_element_type=jnp.float32)
        u = lax.dot_general(x, wu[cols, :], NT, preferred_element_type=jnp.float32)
        hidden[:, cols] = (g / (1.0 + jnp.exp(-g)) * u).astype(jnp.bfloat16)
    split = kept.shape[0]
    h = hidden[...]
    for j in range(0, width, CUT):
        cols = slice(j, min(j + CUT, width))
        y = jnp.dot(h, wd[:, cols], preferred_element_type=jnp.float32)
        kept[:, cols] = y[:split]
        given[:, cols] = y[split:].astype(jnp.bfloat16)


def ffn(own, other, w_gate, w_up, w_down):
    hid, width = w_gate.shape
    n_own, n_other = (sum(b.shape[0] for b in group) for group in (own, other))
    total = n_own + n_other
    blocks = [*own, *other]
    on_chip = pl.BlockSpec(memory_space=pltpu.VMEM)
    return pl.pallas_call(
        functools.partial(ffn_kernel, len(blocks)),
        in_specs=[on_chip] * (len(blocks) + 3),
        out_specs=[on_chip] * 2,
        out_shape=[
            jax.ShapeDtypeStruct((n_own, width), jnp.float32),
            jax.ShapeDtypeStruct((n_other, width), jnp.bfloat16),
        ],
        scratch_shapes=[pltpu.VMEM((total, hid), jnp.bfloat16)],
        cost_estimate=pl.CostEstimate(
            flops=6 * total * width * hid,
            bytes_accessed=6 * width * hid + 8 * total * width,
            transcendentals=total * hid,
        ),
        compiler_params=pltpu.CompilerParams(vmem_limit_bytes=10 << 20),
        name="ffn",
    )(*blocks, w_gate, w_up, w_down)


def shares_kernel(experts, routes, gates, out, wide):
    first = lax.div(lax.axis_index("ep"), SPAN)
    wide[...] = jnp.zeros_like(wide)
    for k in range(experts):
        named = routes[...] == lax.rem(first + k, experts)
        share = jnp.where(named, gates[...], jnp.float32(0.0))
        wide[k : k + 1, : routes.shape[1]] = jnp.sum(share, axis=0, keepdims=True)
    out[...] = wide[...].T[: out.shape[0], :]


def shares(routes, gates, experts):
    on_chip = pl.BlockSpec(memory_space=pltpu.VMEM)
    return pl.pallas_call(
        functools.partial(shares_kernel, experts),
        in_specs=[on_chip, on_chip],
        out_specs=on_chip,
        out_shape=jax.ShapeDtypeStruct((routes.shape[1], SPAN), jnp.float32),
        scratch_shapes=[pltpu.VMEM((SPAN, LANES), jnp.float32)],
        compiler_params=pltpu.CompilerParams(vmem_limit_bytes=2 << 20),
        name="shares",
    )(routes, gates)


def close_kernel(ks, rows, base, one, two, arrived, *outs):
    for i, (k, out) in enumerate(zip(ks, outs, strict=True)):
        total = base[k * rows : (k + 1) * rows, :]
        for part, at in ((one, k - 1), (two, k - 1), (arrived, i)):
            total = total + part[at * rows : (at + 1) * rows, :].astype(jnp.float32)
        out[...] = total.astype(jnp.bfloat16)


def close(ks, rows, base, parts, arrived):
    on_chip = pl.BlockSpec(memory_space=pltpu.VMEM)
    out = jax.ShapeDtypeStruct((rows, base.shape[1]), jnp.bfloat16)
    return pl.pallas_call(
        functools.partial(close_kernel, tuple(ks), rows),
        in_specs=[on_chip] * 4,
        out_specs=[on_chip] * len(ks),
        out_shape=[out] * len(ks),
        compiler_params=pltpu.CompilerParams(vmem_limit_bytes=4 << 20),
        name="close",
    )(base, *parts, arrived)


def norm_kernel(n, devices, *refs):
    tokens, base, weight = refs[:3]
    stays, backs, out = refs[3 : 3 + n], refs[3 + n : -1], refs[-1]
    rows, width = tokens.shape
    columns = width // devices
    per_lane_row = LANES // columns
    mine = base[:rows, :]
    for part in stays:
        mine = mine + part[...].astype(jnp.float32)
    z = ALPHA * tokens[...].astype(jnp.float32) + weight[:, :1] * mine
    for k, part in enumerate(backs):
        z = z + weight[:, k + 1 : k + 2] * part[...].astype(jnp.float32)
    mean = jnp.sum(z, axis=1, keepdims=True) / width
    var = jnp.sum(z * z, axis=1, keepdims=True) / width - mean * mean
    normed = (z - mean) * lax.rsqrt(var + LN_EPS)
    deep = rows // per_lane_row
    for d in range(devices):
        piece = normed[:, d * columns : (d + 1) * columns]
        piece = [piece[h * deep : (h + 1) * deep] for h in range(per_lane_row)]
        out[d * deep : (d + 1) * deep, :] = jnp.concatenate(piece, axis=1)


def norm(tokens, base, weight, stays, backs, devices):
    rows, width = tokens.shape
    on_chip = pl.BlockSpec(memory_space=pltpu.VMEM)
    args = (tokens, base, weight, *stays, *backs)
    return pl.pallas_call(
        functools.partial(norm_kernel, len(stays), devices),
        in_specs=[on_chip] * len(args),
        out_specs=on_chip,
        out_shape=jax.ShapeDtypeStruct((rows * width // LANES, LANES), jnp.float32),
        compiler_params=pltpu.CompilerParams(vmem_limit_bytes=8 << 20),
        name="norm",
    )(*args)


def finish_kernel(deep, x, gain, bias, out):
    packed, lanes = x.shape
    columns, tokens = out.shape
    y = (x[...] * gain[...] + bias[...]).astype(jnp.bfloat16)
    spot = lax.broadcasted_iota(jnp.int32, (packed, 1), 0)
    spot = spot + lax.div(spot, deep) * (deep * (lanes // columns - 1))
    lane = lax.broadcasted_iota(jnp.int32, (packed, tokens), 1)
    total = jnp.zeros(out.shape, jnp.float32)
    for h in range(lanes // columns):
        place = jnp.where(lane == spot + h * deep, 1.0, 0.0).astype(jnp.bfloat16)
        total = total + lax.dot_general(
            y[:, h * columns : (h + 1) * columns], place, TN, preferred_element_type=jnp.float32
        )
    out[...] = total.astype(jnp.bfloat16)


def finish(x, rows, gain, bias):
    columns = gain.shape[0]
    fold = LANES // columns
    on_chip = pl.BlockSpec(memory_space=pltpu.VMEM)
    wide = lambda v: jnp.concatenate([v] * fold).reshape(1, LANES)
    return pl.pallas_call(
        functools.partial(finish_kernel, rows // fold),
        in_specs=[on_chip] * 3,
        out_specs=on_chip,
        out_shape=jax.ShapeDtypeStruct((columns, x.size // columns), jnp.bfloat16),
        compiler_params=pltpu.CompilerParams(vmem_limit_bytes=8 << 20),
        name="finish",
    )(x, wide(gain), wide(bias))


def on_device(tokens, routes, gates, w_gate, w_up, w_down, norm_gain, norm_bias):
    rows, _ = tokens.shape
    devices = lax.axis_size("ep")
    experts = devices // SPAN
    peers = list(range(2, SPAN, 2))
    others = range(1, experts)

    def along(x, k):
        return lax.ppermute(
            x, "ep", [(i, (i + k * SPAN) % devices) for i in range(devices)]
        )

    def across(x, m):
        return lax.ppermute(x, "ep", [(i, i ^ m) for i in range(devices)])

    *projections, held = load(w_gate[0].T, w_up[0].T, tokens)
    weights = (*projections, *load(w_down[0]))

    def run(own):
        other = [across(x, 1) for x in own]
        kept, given = ffn(own, other, *weights)
        return kept + across(given, 1).astype(jnp.float32)

    blocks = [held] + [along(tokens, k) for k in others]
    half = experts // 2
    first, second, far = peers
    early = jnp.concatenate(blocks[:half], axis=0)
    late = jnp.concatenate(blocks[half:], axis=0)
    remote = {m: (across(early, m), across(late, m)) for m in (first, second)}
    result = run([early, late])

    upper = across(remote[first][0], second)
    lower = across(remote[second][1], first)

    ahead = range(half, half + experts // 4)
    behind = [k for k in others if k not in ahead]

    def pick(x, ks):
        return jnp.concatenate([x[k * rows : (k + 1) * rows] for k in ks], axis=0)

    summed = {
        m: run(halves).astype(jnp.bfloat16)
        for m, halves in ((first, remote[first]), (second, remote[second]), (far, (upper, lower)))
    }
    put = {m: across(summed[m][rows:], m) for m in (first, second)}
    put_lead = across(pick(summed[far], ahead), far)
    put_tail = across(pick(summed[far], behind), far)

    back = {}
    for ks, arrived in ((ahead, put_lead), (behind, put_tail)):
        sums = close(ks, rows, result, [put[first], put[second]], arrived)
        for k, total in zip(ks, sums, strict=True):
            back[k] = along(total, -k)
    stays = [across(summed[m][:rows], m) for m in peers]

    weight = shares(routes.T, gates.T, experts)
    packed = norm(held, result, weight, stays, [back[k] for k in others], devices)
    packed = lax.all_to_all(packed.reshape(devices, 1, -1), "ep", 0, 0, tiled=True)
    return finish(packed.reshape(-1, LANES), rows, norm_gain, norm_bias).T


def solution(mesh):
    placed = (
        P(("grp", "ep"), None),
        P(("grp", "ep"), None),
        P(("grp", "ep"), None),
        P("ep", None, None),
        P("ep", None, None),
        P("ep", None, None),
        P("ep"),
        P("ep"),
    )
    return jax.shard_map(
        on_device, mesh=mesh, in_specs=placed, out_specs=P("grp", "ep"), check_vma=False
    )
```

```python
import functools

import jax
import jax.numpy as jnp
from jax import lax
from jax.experimental import pallas as pl
from jax.experimental.pallas import tpu as pltpu
from jax.sharding import PartitionSpec as P


SPAN = 8


ALPHA = 8.0**0.25
LN_EPS = 1e-05
TN = (((0,), (0,)), ((), ()))
CUT = 256
CHUNKS = 4
LANES = 128


def load_kernel(n, *refs):
    sources, targets, sems = refs[:n], refs[n : 2 * n], refs[2 * n]
    copies = []
    for i, (source, target) in enumerate(zip(sources, targets, strict=True)):
        step = target.shape[0] // CHUNKS if target.shape[0] % (16 * CHUNKS) == 0 else target.shape[0]
        for c in range(target.shape[0] // step):
            part = pl.ds(c * step, step)
            copies.append(pltpu.make_async_copy(source.at[part], target.at[part], sems.at[i, c]))
    for copy in copies:
        copy.start()
    for copy in copies:
        copy.wait()


def load(*arrays):
    n = len(arrays)
    arrays = [pltpu.with_memory_space_constraint(x, pltpu.HBM) for x in arrays]
    return pl.pallas_call(
        functools.partial(load_kernel, n),
        in_specs=[pl.BlockSpec(memory_space=pltpu.HBM)] * n,
        out_specs=[pl.BlockSpec(memory_space=pltpu.VMEM)] * n,
        out_shape=[jax.ShapeDtypeStruct(x.shape, x.dtype) for x in arrays],
        scratch_shapes=[pltpu.SemaphoreType.DMA((n, CHUNKS))],
        compiler_params=pltpu.CompilerParams(vmem_limit_bytes=2 << 20),
        name="load",
    )(*arrays)


def turn_kernel(n, *refs):
    for source, target in zip(refs[:n], refs[n:], strict=True):
        hid, width = source.shape
        whole = hid // LANES * LANES
        for j in range(0, width, CUT):
            rows = slice(j, min(j + CUT, width))
            target[rows, :whole] = source[:whole, rows].T
            if whole < hid:
                target[rows, whole:] = source[whole:, rows].T


def turn(*arrays):
    on_chip = pl.BlockSpec(memory_space=pltpu.VMEM)
    return pl.pallas_call(
        functools.partial(turn_kernel, len(arrays)),
        in_specs=[on_chip] * len(arrays),
        out_specs=[on_chip] * len(arrays),
        out_shape=[jax.ShapeDtypeStruct(x.shape[::-1], x.dtype) for x in arrays],
        compiler_params=pltpu.CompilerParams(vmem_limit_bytes=4 << 20),
        name="turn",
    )(*arrays)


def ffn_kernel(n, *refs):
    blocks, (wg, wu, wd, kept, given, hidden) = refs[:n], refs[n:]
    width, hid = wg.shape
    x = jnp.concatenate([b[...] for b in blocks], axis=0)
    for j in range(0, hid, CUT):
        cols = slice(j, min(j + CUT, hid))
        g = jnp.dot(x, wg[:, cols], preferred_element_type=jnp.float32)
        u = jnp.dot(x, wu[:, cols], preferred_element_type=jnp.float32)
        hidden[:, cols] = (g / (1.0 + jnp.exp(-g)) * u).astype(jnp.bfloat16)
    split = kept.shape[0]
    h = hidden[...]
    for j in range(0, width, CUT):
        cols = slice(j, min(j + CUT, width))
        y = jnp.dot(h, wd[:, cols], preferred_element_type=jnp.float32)
        kept[:, cols] = y[:split]
        given[:, cols] = y[split:].astype(jnp.bfloat16)


def ffn(own, other, w_gate, w_up, w_down):
    width, hid = w_gate.shape
    n_own, n_other = (sum(b.shape[0] for b in group) for group in (own, other))
    total = n_own + n_other
    blocks = [*own, *other]
    on_chip = pl.BlockSpec(memory_space=pltpu.VMEM)
    return pl.pallas_call(
        functools.partial(ffn_kernel, len(blocks)),
        in_specs=[on_chip] * (len(blocks) + 3),
        out_specs=[on_chip] * 2,
        out_shape=[
            jax.ShapeDtypeStruct((n_own, width), jnp.float32),
            jax.ShapeDtypeStruct((n_other, width), jnp.bfloat16),
        ],
        scratch_shapes=[pltpu.VMEM((total, hid), jnp.bfloat16)],
        cost_estimate=pl.CostEstimate(
            flops=6 * total * width * hid,
            bytes_accessed=6 * width * hid + 8 * total * width,
            transcendentals=total * hid,
        ),
        compiler_params=pltpu.CompilerParams(vmem_limit_bytes=10 << 20),
        name="ffn",
    )(*blocks, w_gate, w_up, w_down)


def shares_kernel(experts, routes, gates, out, wide):
    first = lax.div(lax.axis_index("ep"), SPAN)
    wide[...] = jnp.zeros_like(wide)
    for k in range(experts):
        named = routes[...] == lax.bitwise_xor(first, k)
        share = jnp.where(named, gates[...], jnp.float32(0.0))
        wide[k : k + 1, : routes.shape[1]] = jnp.sum(share, axis=0, keepdims=True)
    out[...] = wide[...].T[: out.shape[0], :]


def shares(routes, gates, experts):
    on_chip = pl.BlockSpec(memory_space=pltpu.VMEM)
    return pl.pallas_call(
        functools.partial(shares_kernel, experts),
        in_specs=[on_chip, on_chip],
        out_specs=on_chip,
        out_shape=jax.ShapeDtypeStruct((routes.shape[1], SPAN), jnp.float32),
        scratch_shapes=[pltpu.VMEM((SPAN, LANES), jnp.float32)],
        compiler_params=pltpu.CompilerParams(vmem_limit_bytes=2 << 20),
        name="shares",
    )(routes, gates)


def close_kernel(ks, rows, base, one, two, arrived, *outs):
    for i, (k, out) in enumerate(zip(ks, outs, strict=True)):
        total = base[k * rows : (k + 1) * rows, :]
        for part, at in ((one, k - 1), (two, k - 1), (arrived, i)):
            total = total + part[at * rows : (at + 1) * rows, :].astype(jnp.float32)
        out[...] = total.astype(jnp.bfloat16)


def close(ks, rows, base, parts, arrived):
    on_chip = pl.BlockSpec(memory_space=pltpu.VMEM)
    out = jax.ShapeDtypeStruct((rows, base.shape[1]), jnp.bfloat16)
    return pl.pallas_call(
        functools.partial(close_kernel, tuple(ks), rows),
        in_specs=[on_chip] * 4,
        out_specs=[on_chip] * len(ks),
        out_shape=[out] * len(ks),
        compiler_params=pltpu.CompilerParams(vmem_limit_bytes=4 << 20),
        name="close",
    )(base, *parts, arrived)


def norm_kernel(n, devices, *refs):
    tokens, base, weight = refs[:3]
    stays, backs, out = refs[3 : 3 + n], refs[3 + n : -1], refs[-1]
    rows, width = tokens.shape
    columns = width // devices
    per_lane_row = LANES // columns
    mine = base[:rows, :]
    for part in stays:
        mine = mine + part[...].astype(jnp.float32)
    z = ALPHA * tokens[...].astype(jnp.float32) + weight[:, :1] * mine
    for k, part in enumerate(backs):
        z = z + weight[:, k + 1 : k + 2] * part[...].astype(jnp.float32)
    mean = jnp.sum(z, axis=1, keepdims=True) / width
    var = jnp.sum(z * z, axis=1, keepdims=True) / width - mean * mean
    normed = (z - mean) * lax.rsqrt(var + LN_EPS)
    deep = rows // per_lane_row
    for d in range(devices):
        piece = normed[:, d * columns : (d + 1) * columns]
        piece = [piece[h * deep : (h + 1) * deep] for h in range(per_lane_row)]
        out[d * deep : (d + 1) * deep, :] = jnp.concatenate(piece, axis=1)


def norm(tokens, base, weight, stays, backs, devices):
    rows, width = tokens.shape
    on_chip = pl.BlockSpec(memory_space=pltpu.VMEM)
    args = (tokens, base, weight, *stays, *backs)
    return pl.pallas_call(
        functools.partial(norm_kernel, len(stays), devices),
        in_specs=[on_chip] * len(args),
        out_specs=on_chip,
        out_shape=jax.ShapeDtypeStruct((rows * width // LANES, LANES), jnp.float32),
        compiler_params=pltpu.CompilerParams(vmem_limit_bytes=8 << 20),
        name="norm",
    )(*args)


def finish_kernel(deep, x, gain, bias, out):
    packed, lanes = x.shape
    columns, tokens = out.shape
    y = (x[...] * gain[...] + bias[...]).astype(jnp.bfloat16)
    spot = lax.broadcasted_iota(jnp.int32, (packed, 1), 0)
    spot = spot + lax.div(spot, deep) * (deep * (lanes // columns - 1))
    lane = lax.broadcasted_iota(jnp.int32, (packed, tokens), 1)
    total = jnp.zeros(out.shape, jnp.float32)
    for h in range(lanes // columns):
        place = jnp.where(lane == spot + h * deep, 1.0, 0.0).astype(jnp.bfloat16)
        total = total + lax.dot_general(
            y[:, h * columns : (h + 1) * columns], place, TN, preferred_element_type=jnp.float32
        )
    out[...] = total.astype(jnp.bfloat16)


def finish(x, rows, gain, bias):
    columns = gain.shape[0]
    fold = LANES // columns
    on_chip = pl.BlockSpec(memory_space=pltpu.VMEM)
    wide = lambda v: jnp.concatenate([v] * fold).reshape(1, LANES)
    return pl.pallas_call(
        functools.partial(finish_kernel, rows // fold),
        in_specs=[on_chip] * 3,
        out_specs=on_chip,
        out_shape=jax.ShapeDtypeStruct((columns, x.size // columns), jnp.bfloat16),
        compiler_params=pltpu.CompilerParams(vmem_limit_bytes=8 << 20),
        name="finish",
    )(x, wide(gain), wide(bias))


def on_device(tokens, routes, gates, w_gate, w_up, w_down, norm_gain, norm_bias):
    rows, _ = tokens.shape
    devices = lax.axis_size("ep")
    experts = devices // SPAN
    peers = list(range(2, SPAN, 2))
    others = range(1, experts)

    def along(x, k):
        return lax.ppermute(x, "ep", [(i, i ^ (k * SPAN)) for i in range(devices)])

    def across(x, m):
        return lax.ppermute(x, "ep", [(i, i ^ m) for i in range(devices)])

    *projections, held = load(w_gate[0].T, w_up[0].T, tokens)
    projections = turn(*projections)
    weights = (*projections, *load(w_down[0]))

    def run(own):
        other = [across(x, 1) for x in own]
        kept, given = ffn(own, other, *weights)
        return kept + across(given, 1).astype(jnp.float32)

    blocks = [held] + [along(tokens, k) for k in others]
    half = experts // 2
    first, second, far = peers
    early = jnp.concatenate(blocks[:half], axis=0)
    late = jnp.concatenate(blocks[half:], axis=0)
    remote = {m: (across(early, m), across(late, m)) for m in (first, second)}
    result = run([early, late])

    upper = across(remote[first][0], second)
    lower = across(remote[second][1], first)

    ahead = range(half, half + experts // 4)
    behind = [k for k in others if k not in ahead]

    def pick(x, ks):
        return jnp.concatenate([x[k * rows : (k + 1) * rows] for k in ks], axis=0)

    summed = {
        m: run(halves).astype(jnp.bfloat16)
        for m, halves in ((first, remote[first]), (second, remote[second]), (far, (upper, lower)))
    }
    put = {m: across(summed[m][rows:], m) for m in (first, second)}
    put_lead = across(pick(summed[far], ahead), far)
    put_tail = across(pick(summed[far], behind), far)

    back = {}
    for ks, arrived in ((ahead, put_lead), (behind, put_tail)):
        sums = close(ks, rows, result, [put[first], put[second]], arrived)
        for k, total in zip(ks, sums, strict=True):
            back[k] = along(total, k)
    stays = [across(summed[m][:rows], m) for m in peers]

    weight = shares(routes.T, gates.T, experts)
    packed = norm(held, result, weight, stays, [back[k] for k in others], devices)
    packed = lax.all_to_all(packed.reshape(devices, 1, -1), "ep", 0, 0, tiled=True)
    return finish(packed.reshape(-1, LANES), rows, norm_gain, norm_bias).T


def solution(mesh):
    placed = (
        P(("grp", "ep"), None),
        P(("grp", "ep"), None),
        P(("grp", "ep"), None),
        P("ep", None, None),
        P("ep", None, None),
        P("ep", None, None),
        P("ep"),
        P("ep"),
    )
    return jax.shard_map(
        on_device, mesh=mesh, in_specs=placed, out_specs=P("grp", "ep"), check_vma=False
    )
```
